32 devices in a mesh: sp: 8 (over z, x), tp: 4 (over y, core).
Axes of the slice: x: 2, y: 2, z: 4, core: 2. Of those that a mesh axis runs over, the one named last changes fastest.
Arguments:
- resid: bfloat16 [2048, 2048], P(('sp', 'tp')), may hold values from -6 to 6
- query_wide: bfloat16 [2048, 768], P('sp', 'tp'), may hold values from -2000 to 2000
- query_narrow: bfloat16 [2048, 512], P('sp', 'tp'), may hold values from -2000 to 2000
- latent: bfloat16 [2048, 256], P('sp'), may hold values from -6 to 6
- rope_key: bfloat16 [2048, 64], P('sp'), may hold values from -6 to 6
- latent_gain: float32 [256], replicated, may hold values from 0.1 to 1.9
- key_up_wide: bfloat16 [256, 512], replicated, may hold values from -0.375 to 0.375
- value_up_wide: bfloat16 [256, 512], replicated, may hold values from -0.375 to 0.375
- key_up_narrow: bfloat16 [256, 256], replicated, may hold values from -0.375 to 0.375
- value_up_narrow: bfloat16 [256, 256], replicated, may hold values from -0.375 to 0.375
- out_wide: bfloat16 [512, 2048], P('tp'), may hold values from -0.21875 to 0.21875
- out_narrow: bfloat16 [256, 2048], P('tp'), may hold values from -0.21875 to 0.21875
- attn_gain: float32 [2048], replicated, may hold values from 0.1 to 1.9
- ffn_gain: float32 [2048], replicated, may hold values from 0.1 to 1.9
- moe_gain: float32 [2048], replicated, may hold values from 0.1 to 1.9
- routes: int32 [2048, 2], P(('sp', 'tp')), may hold values from 0 to 7, all different within a row; in each aligned block of 64 rows (0 to 63, 64 to 127, ...) at most 24 rows name the same one
- route_logit: float32 [2048, 2], P(('sp', 'tp')), may hold values from -8 to 8
- expert_gate: bfloat16 [8, 2048, 3584], P('sp', None, 'tp'), may hold values from -0.125 to 0.125
- expert_up: bfloat16 [8, 2048, 3584], P('sp', None, 'tp'), may hold values from -0.125 to 0.125
- expert_down: bfloat16 [8, 3584, 2048], P('sp', 'tp'), may hold values from -0.09375 to 0.09375
Outputs:
- mixed: bfloat16 [2048, 2048], P(('sp', 'tp'))
The draws below stay inside these ranges and needn't reach their ends.
Inputs may be any that keep to these rules, and one draw needn't show every extreme that they name: `routes`: in each aligned block of 64 rows no expert is named by more than 24 rows, and a row's experts differ.
All inputs are finite; a program needn't handle non-finite values.
Results may differ from the reference program's by a relative error of at most 0.033.
Values may be sent and summed in bfloat16 or wider, within the bound.
No kernel may reach another device: no remote copies, remote signals or barrier semaphores. Data moves between devices by JAX's collectives and lax.ppermute only.
A program may use at most 128 MiB of HBM per device.

```python
import math
import jax
import jax.numpy as jnp
import numpy as np
from jax import lax

D = 2048
HW = 4
HN = 4
NOPE_W = 128
V_W = 128
NOPE_N = 64
V_N = 64
ROPE = 64
KVR = 256
EFF = 3584
TOP = 2
SEQ = 2048
ROWS = 64
EXPERTS = 8
CAP = 24
N_TP = 4


def spiked(key, row_count, col_count):
    base = jnp.clip(jax.random.normal(key, (row_count, col_count), jnp.float32), -6.0, 6.0)
    return base.astype(jnp.bfloat16)


def draw_query_wide(key, part):
    return spiked(jax.random.fold_in(key, 11), SEQ, HW * (NOPE_W + ROPE))


def draw_query_narrow(key, part):
    return spiked(jax.random.fold_in(key, 13), SEQ, HN * (NOPE_N + ROPE))


def block_scale(stream_key, dims, split, smallest, top_value):
    level = 1.0
    for axis_at, blocks in split:
        steps = jax.random.uniform(jax.random.fold_in(jax.random.fold_in(stream_key, 6), axis_at), (blocks,), jnp.float32, smallest / len(split), top_value / len(split))
        level = level * jnp.repeat(jnp.exp(steps), dims[axis_at] // blocks).reshape((-1,) + (1,) * (len(dims) - 1 - axis_at))
    return level


def deal_out(stream_key, own, number, rows, number_of, top, bound, skew):
    order = jax.random.permutation(stream_key, number_of)
    packed, ordinary = portions_of(number_of, rows * top, bound, skew, True), portions_of(number_of, rows * top, bound, skew, False)
    places = jnp.arange(number_of)

    def named(tallies, offset_by):
        used = int((tallies > 0).sum())
        fixed = max(1, used // 4)
        moved = fixed + (places - fixed + offset_by * (used - fixed)) % max(1, number_of - fixed)
        return jnp.zeros((number_of,), jnp.int32).at[order[jnp.where(places < fixed, places, moved)]].set(jnp.asarray(tallies, jnp.int32))

    tallies = jnp.where(number % 4 == 0, named(packed, number // 4), named(ordinary, number - number // 4 - 1))
    mixed = jax.random.permutation(jax.random.fold_in(own, 3), number_of)
    giver, taker = mixed[0:number_of // 2 * 2:2], mixed[1:number_of // 2 * 2:2]
    room = jnp.minimum(tallies[giver] - 1, bound - tallies[taker]) // 2
    room = jnp.where((giver == order[0]) | (taker == order[0]) | (tallies[taker] == 0), 0, jnp.maximum(room, 0))
    moved = jax.random.randint(jax.random.fold_in(own, 4), (number_of // 2,), 0, 1 << 20) % (room + 1)
    tallies = tallies.at[giver].add(-moved).at[taker].add(moved)
    items = jnp.searchsorted(jnp.cumsum(tallies), jnp.arange(rows * top), side="right").astype(jnp.int32)
    listing = items.reshape(top, rows).T
    listing = listing[jax.random.permutation(jax.random.fold_in(own, 1), rows)]
    offset_by = jax.random.randint(jax.random.fold_in(own, 2), (rows, 1), 0, top)
    return jnp.take_along_axis(listing, (jnp.arange(top)[None, :] + offset_by) % top, axis=1)


def portions_of(count, total, most, skew, full):
    portions = [(1 << 20) // math.isqrt(grade ** skew) + 1 for grade in range(1, count + 1)]
    largest = most if full else min(most, max(-(-total // count), total * portions[0] // sum(portions)))
    least = 1 if total - largest >= count - 1 else 0
    counts, surplus = [largest] + [least] * (count - 1), total - largest - least * (count - 1)
    while surplus > 0:
        free = [i for i in range(1, count) if counts[i] < largest] or [i for i in range(1, count) if counts[i] < most]
        whole, left = sum([portions[i] for i in free]), surplus
        for i in free:
            extra = min(most - counts[i], max(1, left * portions[i] // whole), surplus)
            counts[i] = counts[i] + extra
            surplus = surplus - extra
    return np.array(counts)


def normal_values(key, extent, scale, most, pieces=(), kind=jnp.bfloat16):
    array = jax.random.normal(key, extent, jnp.float32) * scale
    if len(pieces) > 0:
        array = block_scale(key, extent, pieces, -0.22, 0.18) * array
    return jnp.clip(array, min=-most, max=most).astype(kind)


def setup_inputs(seed: int = 0) -> dict:
    seeds = jax.random.split(jax.random.key(seed), 21)
    resid = normal_values(seeds[0], (SEQ, D), 1.0, 6.0, ((0, 32),))
    query_wide = draw_query_wide(jax.random.fold_in(seeds[20], 71), 0)
    query_narrow = draw_query_narrow(jax.random.fold_in(seeds[20], 71), 0)
    latent = normal_values(seeds[3], (SEQ, KVR), 1.0, 6.0, ((0, 8),))
    rope_key = normal_values(seeds[4], (SEQ, ROPE), 1.0, 6.0, ((0, 8),))
    latent_gain = jnp.clip(1.0 + 0.18 * jax.random.normal(seeds[5], (KVR,), jnp.float32), 0.1, 1.9)
    key_up_wide = normal_values(seeds[6], (KVR, HW * NOPE_W), KVR ** -0.5, 0.375)
    value_up_wide = normal_values(seeds[7], (KVR, HW * V_W), KVR ** -0.5, 0.375)
    key_up_narrow = normal_values(seeds[8], (KVR, HN * NOPE_N), KVR ** -0.5, 0.375)
    value_up_narrow = normal_values(seeds[9], (KVR, HN * V_N), KVR ** -0.5, 0.375)
    out_wide = normal_values(seeds[10], (HW * V_W, D), (HW * V_W + HN * V_N) ** -0.5, 0.21875, ((0, 4),))
    out_narrow = normal_values(seeds[11], (HN * V_N, D), (HW * V_W + HN * V_N) ** -0.5, 0.21875, ((0, 4),))
    attn_gain = jnp.clip(1.0 + 0.18 * jax.random.normal(seeds[12], (D,), jnp.float32), 0.1, 1.9)
    ffn_gain = jnp.clip(1.0 + 0.18 * jax.random.normal(seeds[13], (D,), jnp.float32), 0.1, 1.9)
    moe_gain = jnp.clip(1.0 + 0.18 * jax.random.normal(seeds[14], (D,), jnp.float32), 0.1, 1.9)
    routes_keys = jax.random.split(jax.random.fold_in(seeds[15], 1), SEQ // ROWS)
    routes_turns = jax.random.permutation(jax.random.fold_in(seeds[15], 3), SEQ // ROWS)
    routes = jax.vmap(lambda own, number: deal_out(jax.random.fold_in(seeds[15], 2), own, number, ROWS, EXPERTS, TOP, CAP, 2))(routes_keys, routes_turns).reshape((SEQ, TOP))
    route_logit = normal_values(seeds[16], (SEQ, TOP), 1.5, 8.0, ((0, 32),), jnp.float32)
    expert_gate = normal_values(seeds[17], (EXPERTS, D, EFF), D ** -0.5, 0.125, ((0, 8), (2, 4)))
    expert_up = normal_values(seeds[18], (EXPERTS, D, EFF), D ** -0.5, 0.125, ((0, 8), (2, 4)))
    expert_down = normal_values(seeds[19], (EXPERTS, EFF, D), EFF ** -0.5, 0.09375, ((0, 8), (1, 4)))
    return {"resid": resid, "query_wide": query_wide, "query_narrow": query_narrow, "latent": latent, "rope_key": rope_key, "latent_gain": latent_gain, "key_up_wide": key_up_wide, "value_up_wide": value_up_wide, "key_up_narrow": key_up_narrow, "value_up_narrow": value_up_narrow, "out_wide": out_wide, "out_narrow": out_narrow, "attn_gain": attn_gain, "ffn_gain": ffn_gain, "moe_gain": moe_gain, "routes": routes, "route_logit": route_logit, "expert_gate": expert_gate, "expert_up": expert_up, "expert_down": expert_down}


EPS = 1e-06
THETA = 10000.0

def rms_scale(values, gain):
    return values * lax.rsqrt(lax.optimization_barrier(jnp.mean(values * values, axis=-1, keepdims=True)) + EPS) * gain.astype(jnp.float32)

def rotate(values, positions):
    half = values.shape[-1] // 2
    freq = THETA ** (-jnp.arange(half, dtype=jnp.float32) * 2.0 / values.shape[-1])
    angle = positions.astype(jnp.float32)[..., None] * freq
    cosine = jnp.cos(angle)
    sine = jnp.sin(angle)
    real = values.astype(jnp.float32)
    first = real[..., :half]
    second = real[..., half:]
    return jnp.concatenate([first * cosine - second * sine, second * cosine + first * sine], axis=-1).astype(jnp.bfloat16)

def contract(left, right):
    return lax.dot_general(left, right, (((1,), (1,)), ((), ())), preferred_element_type=jnp.float32)

def head_attend(q_nope, q_rope, k_nope, k_rope, values, factor):
    length = q_nope.shape[0]
    block = math.gcd(length, 512)

    def one_block(index):
        query_a = lax.dynamic_slice_in_dim(q_nope, index * block, block, 0)
        query_b = lax.dynamic_slice_in_dim(q_rope, index * block, block, 0)
        scores = (contract(query_a, k_nope) + contract(query_b, k_rope)) * factor
        top_score = lax.optimization_barrier(jnp.max(scores, axis=1, keepdims=True))
        weights = jnp.exp(scores - top_score)
        weight_sum = lax.optimization_barrier(jnp.sum(weights, axis=1, keepdims=True))
        summed = jnp.dot(weights.astype(jnp.bfloat16), values, preferred_element_type=jnp.float32)
        return (summed / weight_sum).astype(jnp.bfloat16)
    blocks = jnp.arange(length // block, dtype=jnp.int32)
    result = lax.map(one_block, blocks)
    return result.reshape(length, values.shape[1])

def rounded(values):
    return lax.optimization_barrier(values.astype(jnp.bfloat16)).astype(jnp.float32)

def reference(resid, query_wide, query_narrow, latent, rope_key, latent_gain, key_up_wide, value_up_wide, key_up_narrow, value_up_narrow, out_wide, out_narrow, attn_gain, ffn_gain, moe_gain, routes, route_logit, expert_gate, expert_up, expert_down):
    positions = jnp.arange(SEQ, dtype=jnp.int32)
    normed = rms_scale(latent.astype(jnp.float32), latent_gain).astype(jnp.bfloat16)
    turned_key = rotate(rope_key, positions)

    def expand(weight):
        return jnp.dot(normed, weight, preferred_element_type=jnp.float32).astype(jnp.bfloat16)
    keys_wide = expand(key_up_wide)
    vals_wide = expand(value_up_wide)
    keys_narrow = expand(key_up_narrow)
    vals_narrow = expand(value_up_narrow)
    q_wide = query_wide.reshape(SEQ, HW, NOPE_W + ROPE)
    q_narrow = query_narrow.reshape(SEQ, HN, NOPE_N + ROPE)
    wide_turn = rotate(q_wide[:, :, NOPE_W:], positions[:, None])
    narrow_turn = rotate(q_narrow[:, :, NOPE_N:], positions[:, None])
    wide_outs = []
    for head in range(HW):
        wide_outs.append(head_attend(q_wide[:, head, :NOPE_W], wide_turn[:, head], keys_wide[:, head * NOPE_W:(head + 1) * NOPE_W], turned_key, vals_wide[:, head * V_W:(head + 1) * V_W], (NOPE_W + ROPE) ** (-0.5)))
    narrow_outs = []
    for head in range(HN):
        narrow_outs.append(head_attend(q_narrow[:, head, :NOPE_N], narrow_turn[:, head], keys_narrow[:, head * NOPE_N:(head + 1) * NOPE_N], turned_key, vals_narrow[:, head * V_N:(head + 1) * V_N], (NOPE_N + ROPE) ** (-0.5)))
    o_wide = jnp.concatenate(wide_outs, axis=1)
    o_narrow = jnp.concatenate(narrow_outs, axis=1)
    wide_cols = HW // N_TP * V_W
    narrow_cols = HN // N_TP * V_N
    proj = jnp.zeros((SEQ, D), jnp.float32)
    for group in range(N_TP):
        part = jnp.dot(o_wide[:, group * wide_cols:(group + 1) * wide_cols], out_wide[group * wide_cols:(group + 1) * wide_cols], preferred_element_type=jnp.float32)
        part = part + jnp.dot(o_narrow[:, group * narrow_cols:(group + 1) * narrow_cols], out_narrow[group * narrow_cols:(group + 1) * narrow_cols], preferred_element_type=jnp.float32)
        proj = proj + rounded(part)
    stream = (resid.astype(jnp.float32) + rms_scale(proj, attn_gain)).astype(jnp.bfloat16)
    moe_in = rms_scale(stream.astype(jnp.float32), ffn_gain).astype(jnp.bfloat16)
    n_blocks = SEQ // ROWS
    pairs = ROWS * TOP
    chosen = routes.reshape(n_blocks, pairs)
    onehot = (chosen[:, :, None] == jnp.arange(EXPERTS, dtype=jnp.int32)[None, None, :]).astype(jnp.int32)
    before = jnp.cumsum(onehot, axis=1) - onehot
    slot = lax.optimization_barrier(jnp.sum(before * onehot, axis=2))
    dest = (chosen * CAP + slot).astype(jnp.int32)
    row_index = (jnp.arange(n_blocks, dtype=jnp.int32)[:, None] * ROWS + jnp.arange(pairs, dtype=jnp.int32)[None, :] // TOP).astype(jnp.int32)
    table = jnp.full((n_blocks, EXPERTS * CAP), -1, jnp.int32)
    table = table.at[jnp.arange(n_blocks, dtype=jnp.int32)[:, None], dest].set(row_index)
    per_expert = jnp.transpose(table.reshape(n_blocks, EXPERTS, CAP), (1, 0, 2)).reshape(EXPERTS, n_blocks * CAP)
    width = EFF // N_TP

    def one_expert(operands):
        index, w_gate, w_up, w_down = operands
        picked = moe_in[jnp.maximum(index, 0)]
        picked = jnp.where((index >= 0)[:, None], picked, jnp.zeros_like(picked))
        summed = jnp.zeros((index.shape[0], D), jnp.float32)
        for group in range(N_TP):
            gate = jnp.dot(picked, w_gate[:, group * width:(group + 1) * width], preferred_element_type=jnp.float32)
            upper = jnp.dot(picked, w_up[:, group * width:(group + 1) * width], preferred_element_type=jnp.float32)
            hidden = (jax.nn.silu(gate) * upper).astype(jnp.bfloat16)
            part = jnp.dot(hidden, w_down[group * width:(group + 1) * width], preferred_element_type=jnp.float32)
            summed = summed + rounded(part)
        return summed.astype(jnp.bfloat16)
    expert_out = lax.map(one_expert, (per_expert, expert_gate, expert_up, expert_down))
    by_block = jnp.transpose(expert_out.reshape(EXPERTS, n_blocks, CAP, D), (1, 0, 2, 3)).reshape(n_blocks, EXPERTS * CAP, D)
    gathered = by_block[jnp.arange(n_blocks, dtype=jnp.int32)[:, None], dest].reshape(SEQ, TOP, D)
    share = jax.nn.softmax(route_logit.astype(jnp.float32), axis=-1)
    branch = lax.optimization_barrier(jnp.sum(share[:, :, None] * gathered.astype(jnp.float32), axis=1))
    return (stream.astype(jnp.float32) + rms_scale(branch, moe_gain)).astype(jnp.bfloat16)
```

```python
import functools

import jax
import jax.numpy as jnp
import numpy as np
from jax import lax
from jax.experimental import pallas as pl
from jax.experimental.pallas import tpu as pltpu
from jax.sharding import PartitionSpec as P

NOPE_W = 128
V_W = 128
NOPE_N = 64
V_N = 64
ROPE = 64

EPS = 1e-06
THETA = 10000.0
LOG2E = 1.4426950408889634
BF16 = jnp.bfloat16
F32 = jnp.float32


def rms_scale(values, gain):
    return values * lax.rsqrt(jnp.mean(values * values, axis=-1, keepdims=True) + EPS) * gain


def rotate(values, positions):
    half = values.shape[-1] // 2
    freq = THETA ** (-jnp.arange(half, dtype=jnp.float32) * 2.0 / values.shape[-1])
    angle = positions.astype(jnp.float32)[..., None] * freq
    cosine = jnp.cos(angle)
    sine = jnp.sin(angle)
    real = values.astype(jnp.float32)
    first = real[..., :half]
    second = real[..., half:]
    return jnp.concatenate(
        [first * cosine - second * sine, second * cosine + first * sine], axis=-1
    ).astype(jnp.bfloat16)


def contract(left, right):
    return lax.dot_general(
        left, right, (((1,), (1,)), ((), ())), preferred_element_type=jnp.float32
    )


def attend(q_nope, q_rope, k_nope, k_rope, values, factor):
    scores = (contract(q_nope, k_nope) + contract(q_rope, k_rope)) * factor
    top = jnp.max(scores, axis=1, keepdims=True)
    weights = jnp.exp(scores - top)
    weight_sum = jnp.sum(weights, axis=1, keepdims=True)
    summed = jnp.dot(weights.astype(BF16), values, preferred_element_type=F32)
    return (summed / weight_sum).astype(BF16)


def local_plain(
    resid,
    query_wide,
    query_narrow,
    latent,
    rope_key,
    latent_gain,
    key_up_wide,
    value_up_wide,
    key_up_narrow,
    value_up_narrow,
    out_wide,
    out_narrow,
    attn_gain,
    ffn_gain,
    moe_gain,
    routes,
    route_logit,
    expert_gate,
    expert_up,
    expert_down,
):
    tok_rows = latent.shape[0]
    wide_heads = query_wide.shape[1] // (NOPE_W + ROPE)
    narrow_heads = query_narrow.shape[1] // (NOPE_N + ROPE)
    tp_rank = lax.axis_index("tp")
    positions = lax.axis_index("sp") * tok_rows + jnp.arange(tok_rows, dtype=jnp.int32)
    normed = rms_scale(latent.astype(jnp.float32), latent_gain).astype(jnp.bfloat16)
    turned_key = rotate(rope_key, positions)

    def my_columns(weight, count):
        return lax.dynamic_slice_in_dim(weight, tp_rank * count, count, 1)

    latent_rows = lax.all_gather(normed, "sp", axis=0, tiled=True)
    turned_rows = lax.all_gather(turned_key, "sp", axis=0, tiled=True)

    def expand(weight, count):
        return jnp.dot(
            latent_rows, my_columns(weight, count), preferred_element_type=F32
        ).astype(BF16)

    def group(query, heads, nope, value, key_up, value_up):
        query = query.reshape(tok_rows, heads, nope + ROPE)
        turned = rotate(query[:, :, nope:], positions[:, None])
        keys = expand(key_up, heads * nope)
        values = expand(value_up, heads * value)
        return [
            attend(
                query[:, h, :nope],
                turned[:, h],
                keys[:, h * nope : (h + 1) * nope],
                turned_rows,
                values[:, h * value : (h + 1) * value],
                (nope + ROPE) ** (-0.5),
            )
            for h in range(heads)
        ]

    wide_out = jnp.concatenate(
        group(query_wide, wide_heads, NOPE_W, V_W, key_up_wide, value_up_wide), axis=1
    )
    narrow_out = jnp.concatenate(
        group(query_narrow, narrow_heads, NOPE_N, V_N, key_up_narrow, value_up_narrow), axis=1
    )
    row_count = resid.shape[0]
    proj = lax.psum_scatter(
        (
            jnp.dot(wide_out, out_wide, preferred_element_type=jnp.float32)
            + jnp.dot(narrow_out, out_narrow, preferred_element_type=jnp.float32)
        ).astype(jnp.bfloat16),
        "tp",
        scatter_dimension=0,
        tiled=True,
    ).astype(jnp.float32)
    stream = (resid.astype(jnp.float32) + rms_scale(proj, attn_gain)).astype(jnp.bfloat16)
    moe_in = rms_scale(stream.astype(jnp.float32), ffn_gain).astype(jnp.bfloat16)
    top_count = routes.shape[1]
    experts = lax.axis_size("sp")
    capacity = (3 * row_count * top_count + 2 * experts - 1) // (2 * experts)
    chosen = routes.reshape(-1)
    onehot = (chosen[:, None] == jnp.arange(experts, dtype=jnp.int32)[None, :]).astype(jnp.int32)
    before = jnp.cumsum(onehot, axis=0) - onehot
    slot = jnp.sum(before * onehot, axis=1)
    dest = (chosen * capacity + slot).reshape(row_count, top_count)
    slot_ids = jnp.arange(experts * capacity, dtype=jnp.int32)
    placing = jnp.any(slot_ids[:, None, None] == dest[None, :, :], axis=2).astype(jnp.bfloat16)
    outgoing = jnp.dot(placing, moe_in, preferred_element_type=jnp.float32).astype(jnp.bfloat16)
    outgoing = outgoing.reshape(experts, capacity, moe_in.shape[1])
    gathered = lax.all_gather(
        lax.all_to_all(outgoing, "sp", split_axis=0, concat_axis=0, tiled=True),
        "tp",
        axis=0,
        tiled=True,
    )
    flat = gathered.reshape(-1, gathered.shape[2])
    gate = jnp.dot(flat, expert_gate[0], preferred_element_type=jnp.float32)
    upper = jnp.dot(flat, expert_up[0], preferred_element_type=jnp.float32)
    hidden = (jax.nn.silu(gate) * upper).astype(jnp.bfloat16)
    partial_out = jnp.dot(hidden, expert_down[0], preferred_element_type=jnp.float32).reshape(
        gathered.shape
    )
    summed = lax.psum_scatter(
        partial_out.astype(jnp.bfloat16), "tp", scatter_dimension=0, tiled=True
    )
    returned = lax.all_to_all(summed, "sp", split_axis=0, concat_axis=0, tiled=True)
    flat_back = returned.reshape(experts * capacity, returned.shape[2])
    picked = flat_back[dest]
    share = jax.nn.softmax(route_logit, axis=-1)
    branch = jnp.sum(share[:, :, None] * picked.astype(jnp.float32), axis=1)
    return (stream.astype(jnp.float32) + rms_scale(branch, moe_gain)).astype(jnp.bfloat16)


def dot(left, right):
    return jnp.dot(left, right, preferred_element_type=F32)


def sds(shape, dtype=BF16):
    return jax.ShapeDtypeStruct(shape, dtype)


VMEM = pl.BlockSpec(memory_space=pltpu.VMEM)
ANY = pl.BlockSpec(memory_space=pl.ANY)


def call(body, outs, ins, *args, scratch=(), name, flops=10**8, data=10**6, limit=None):
    return pl.pallas_call(
        body,
        out_shape=outs,
        in_specs=ins,
        out_specs=jax.tree.map(lambda _: VMEM, outs),
        scratch_shapes=list(scratch),
        name=name,
        cost_estimate=pl.CostEstimate(flops=flops, bytes_accessed=data, transcendentals=0),
        compiler_params=pltpu.CompilerParams(vmem_limit_bytes=limit),
    )(*args)


def angles(freq, start, count):
    spots = start + lax.broadcasted_iota(jnp.int32, (freq.shape[0], count), 1)
    return spots.astype(F32) * freq


def turn_rows(block, cosine, sine):
    half = block.shape[0] // 2
    first, second = block[:half], block[half:]
    return first * cosine - second * sine, second * cosine + first * sine


def pack_body(latent, rope, gain, freq, out):
    half = latent.shape[0] // 2
    base = pl.multiple_of((lax.axis_index("tp") % 2) * half, half)
    rows = latent[pl.ds(base, half), :].astype(F32)
    out[:half] = rms_scale(rows, gain[...]).astype(BF16)
    angle = angles(freq[...], lax.axis_index("sp") * latent.shape[0] + base, half)
    keys = rope[:, pl.ds(base, half)].astype(F32)
    first, second = turn_rows(keys, jnp.cos(angle), jnp.sin(angle))
    out[half:, :half] = first.astype(BF16)
    out[half:, half:] = second.astype(BF16)


def prepare_body(
    key_wide, value_wide, key_narrow, value_narrow, wide, narrow, freq, info,
    key_up, value_up, turned_wide, turned_narrow, place, weigh,
):
    group = lax.axis_index("tp")
    span = pl.ds(pl.multiple_of(group * NOPE_W, NOPE_W), NOPE_W)
    pair = pl.ds(pl.multiple_of((group // 2) * (2 * NOPE_N), 2 * NOPE_N), 2 * NOPE_N)
    odd = group % 2 == 1

    def narrow_part(ref):
        both = ref[:, pair].astype(F32)
        return jnp.where(odd, both[:, NOPE_N:], both[:, :NOPE_N])

    key_up[:NOPE_W, :] = key_wide[:, span].astype(F32).T.astype(BF16)
    key_up[NOPE_W:, :] = narrow_part(key_narrow).T.astype(BF16)
    value_up[:, :V_W] = value_wide[:, span]
    value_up[:, V_W:] = narrow_part(value_narrow).astype(BF16)
    count = wide.shape[1]
    angle = angles(freq[:, :1], lax.axis_index("sp") * count, count)
    cosine, sine = jnp.cos(angle), jnp.sin(angle)
    for query, nope, out in ((wide, NOPE_W, turned_wide), (narrow, NOPE_N, turned_narrow)):
        first, second = turn_rows(query[nope:, :].astype(F32), cosine, sine)
        full = jnp.concatenate([query[:nope, :].astype(F32), first, second], axis=0)
        out[...] = full.T.astype(BF16)
    experts, capacity, tokens = place.shape
    earlier = (
        lax.broadcasted_iota(jnp.int32, (tokens, tokens), 0)
        < lax.broadcasted_iota(jnp.int32, (tokens, tokens), 1)
    ).astype(F32)
    expert_ids = lax.broadcasted_iota(jnp.int32, (experts, tokens), 0).astype(F32)
    row_ids = lax.broadcasted_iota(jnp.int32, (experts * capacity, tokens), 0)
    named = [(expert_ids == info[k : k + 1, :]).astype(F32) for k in range(2)]
    before = dot(named[0] + named[1], earlier)
    logits = [info[2 + k : 3 + k, :] for k in range(2)]
    top = jnp.maximum(logits[0], logits[1])
    raised = [jnp.exp(item - top) for item in logits]
    total = raised[0] + raised[1]
    placed = jnp.zeros(row_ids.shape, F32)
    weighed = jnp.zeros(row_ids.shape, F32)
    for k in range(2):
        slot = jnp.sum(before * named[k], axis=0, keepdims=True).astype(jnp.int32)
        away = info[k : k + 1, :].astype(jnp.int32) ^ lax.axis_index("sp")
        hit = row_ids == away * capacity + slot
        placed = jnp.where(hit, 1.0, placed)
        weighed = jnp.where(hit, raised[k] / total, weighed)
    place[...] = placed.reshape(place.shape).astype(BF16)
    weigh[...] = weighed.T


def attention_body(*refs, packs):
    blocks = refs[:packs]
    key_up, value_up, wide, narrow = refs[packs : packs + 4]
    outs = refs[packs + 4 : packs + 8]
    normed, keys_w, keys_n, values, held = refs[packs + 8 :]
    half = blocks[0].shape[0] * 4 // 5
    quarter = ROPE // 2
    for j, ref in enumerate(blocks):
        span = pl.ds(j * half, half)
        normed[span, :] = ref[:half, :]
        turned = ref[half:, :]
        for keys, nope in ((keys_w, NOPE_W), (keys_n, NOPE_N)):
            keys[nope : nope + quarter, span] = turned[:, :half]
            keys[nope + quarter : nope + ROPE, span] = turned[:, half:]
    up = contract(key_up[...], normed[...]).astype(BF16)
    keys_w[:NOPE_W, :] = up[:NOPE_W]
    keys_n[:NOPE_N, :] = up[NOPE_W:]
    values[...] = dot(normed[...], value_up[...]).astype(BF16)
    spans = ((wide, keys_w, NOPE_W, 0, V_W), (narrow, keys_n, NOPE_N, V_W, V_W + V_N))
    for query, keys, nope, low, high in spans:
        score = dot(query[...], keys[...])
        top = jnp.max(score, axis=1, keepdims=True)
        weight = jnp.exp2((score - top) * ((nope + ROPE) ** (-0.5) * LOG2E))
        total = jnp.sum(weight, axis=1, keepdims=True)
        summed = dot(weight.astype(BF16), values[:, low:high])
        held[:, low:high] = (summed / total).astype(BF16)
    rows = outs[0].shape[0]
    for k, out in enumerate(outs):
        at = pl.multiple_of((lax.axis_index("tp") ^ k) * rows, rows)
        out[...] = held[pl.ds(at, rows), :]


def project_body(
    o0, o1, o2, o3, w0, w1, w2, w3, resid, attn_gain, ffn_gain, place, stream, *outs
):
    proj = (
        dot(o0[...], w0[...]) + dot(o1[...], w1[...]) + dot(o2[...], w2[...]) + dot(o3[...], w3[...])
    )
    mixed = (resid[...].astype(F32) + rms_scale(proj, attn_gain[...])).astype(BF16)
    stream[...] = mixed
    moved = rms_scale(mixed.astype(F32), ffn_gain[...]).astype(BF16)
    for k, out in enumerate(outs):
        out[...] = dot(place[k], moved).astype(BF16)


def join_body(first, second, out):
    rows = first.shape[0]
    out[:rows] = first[...]
    out[rows:] = second[...]


def expert_body(*refs, blocks, tile, down_tile):
    parts = refs[:blocks]
    gate, up, down = refs[blocks : blocks + 3]
    keep, send = refs[blocks + 3 : blocks + 5]
    rows, gate_v, up_v, down_v, hidden, sem_x, sem_g, sem_u, sem_d = refs[blocks + 5 :]
    size = parts[0].shape[0]
    half = blocks * size // 2
    width = gate.shape[2]
    tiles = [(at, min(tile, width - at)) for at in range(0, width, tile)]
    loads = [
        pltpu.make_async_copy(ref, rows.at[pl.ds(j * size, size)], sem_x.at[j])
        for j, ref in enumerate(parts)
    ]
    pieces = []
    for j, (at, count) in enumerate(tiles):
        span = pl.ds(at, count)
        pieces.append(
            (
                pltpu.make_async_copy(gate.at[0, :, span], gate_v.at[:, span], sem_g.at[j]),
                pltpu.make_async_copy(up.at[0, :, span], up_v.at[:, span], sem_u.at[j]),
            )
        )
    last = pltpu.make_async_copy(down.at[0], down_v, sem_d.at[0])
    for item in pieces[0]:
        item.start()
    for item in loads:
        item.start()
    for pair in pieces[1:]:
        for item in pair:
            item.start()
    last.start()
    for item in loads:
        item.wait()
    for j, (at, count) in enumerate(tiles):
        for item in pieces[j]:
            item.wait()
        span = pl.ds(at, count)
        left = dot(rows[...], gate_v[:, span])
        right = dot(rows[...], up_v[:, span])
        hidden[:, span] = (left * jax.nn.sigmoid(left) * right).astype(BF16)
    last.wait()
    for at in range(0, keep.shape[1], down_tile):
        span = pl.ds(at, down_tile)
        send[:, span] = dot(hidden[half:, :], down_v[:, span]).astype(BF16)
        keep[:, span] = dot(hidden[:half, :], down_v[:, span]).astype(BF16)


def add_body(mine, other, *outs):
    rows = outs[0].shape[0]
    for k, out in enumerate(outs):
        span = pl.ds(k * rows, rows)
        out[...] = (mine[span, :].astype(F32) + other[span, :].astype(F32)).astype(BF16)


def split_body(mine, other, first, second):
    total = (mine[...].astype(F32) + other[...].astype(F32)).astype(BF16)
    rows = first.shape[0]
    first[...] = total[:rows]
    second[...] = total[rows:]


def finish_body(weigh, stream, gain, *refs):
    *blocks, out, full = refs
    rows = blocks[0].shape[0]
    for k, ref in enumerate(blocks):
        full[k * rows : (k + 1) * rows, :] = ref[...]
    whole = weigh[...]
    high = whole.astype(BF16)
    low = (whole - high.astype(F32)).astype(BF16)
    branch = dot(high, full[...]) + dot(low, full[...])
    out[...] = (stream[...].astype(F32) + rms_scale(branch, gain[...])).astype(BF16)


def permuted(value, axis, step):
    size = lax.axis_size(axis)
    return lax.ppermute(value, axis, [(i, i ^ step) for i in range(size)])


def local_permuted(
    resid,
    query_wide,
    query_narrow,
    latent,
    rope_key,
    latent_gain,
    key_up_wide,
    value_up_wide,
    key_up_narrow,
    value_up_narrow,
    out_wide,
    out_narrow,
    attn_gain,
    ffn_gain,
    moe_gain,
    routes,
    route_logit,
    expert_gate,
    expert_up,
    expert_down,
):
    experts = lax.axis_size("sp")
    tokens = latent.shape[0]
    width = resid.shape[1]
    rows = resid.shape[0]
    top_count = routes.shape[1]
    capacity = (3 * rows * top_count + 2 * experts - 1) // (2 * experts)
    half = tokens // 2
    hops = range(experts // 2)
    freq = jnp.asarray(
        np.repeat((THETA ** (-np.arange(ROPE // 2) * 2.0 / ROPE))[:, None], half, 1), F32
    )

    pack = call(
        pack_body,
        sds((half + ROPE // 2, latent.shape[1])),
        [VMEM] * 4,
        latent,
        rope_key.T,
        latent_gain[None, :],
        freq,
        name="pack",
    )
    columns = [pack] + [permuted(pack, "sp", 2 * j) for j in hops[1:]]
    columns += [permuted(item, "sp", 1) for item in columns]
    packs = columns + [permuted(item, "tp", 1) for item in columns]

    own_out = jnp.concatenate([out_wide, out_narrow], axis=0)
    across_out = permuted(own_out, "tp", 2)

    info = jnp.concatenate([routes.T.astype(F32), route_logit.T], axis=0)
    key_up, value_up, turned_wide, turned_narrow, place, weigh = call(
        prepare_body,
        (
            sds((NOPE_W + NOPE_N, latent.shape[1])),
            sds((latent.shape[1], V_W + V_N)),
            sds((tokens, NOPE_W + ROPE)),
            sds((tokens, NOPE_N + ROPE)),
            sds((experts, capacity, rows)),
            sds((rows, experts * capacity), F32),
        ),
        [VMEM] * 8,
        key_up_wide,
        value_up_wide,
        key_up_narrow,
        value_up_narrow,
        query_wide.T,
        query_narrow.T,
        freq,
        info,
        name="prepare",
    )
    everyone = experts * tokens
    heads = call(
        functools.partial(attention_body, packs=2 * experts),
        tuple(sds((rows, V_W + V_N)) for _ in range(4)),
        [VMEM] * (2 * experts + 4),
        *packs,
        key_up,
        value_up,
        turned_wide,
        turned_narrow,
        scratch=[
            pltpu.VMEM((everyone, latent.shape[1]), BF16),
            pltpu.VMEM((NOPE_W + ROPE, everyone), BF16),
            pltpu.VMEM((NOPE_N + ROPE, everyone), BF16),
            pltpu.VMEM((everyone, V_W + V_N), BF16),
            pltpu.VMEM((tokens, V_W + V_N), BF16),
        ],
        name="attention",
        flops=10**9,
    )
    across_out, *heads = lax.optimization_barrier((across_out, *heads))
    outs = [own_out, permuted(own_out, "tp", 1), across_out, permuted(across_out, "tp", 1)]
    heads = [heads[0]] + [permuted(heads[k], "tp", k) for k in range(1, 4)]
    stream, *outgoing = call(
        project_body,
        (sds((rows, width)),) + tuple(sds((capacity, width)) for _ in range(experts)),
        [VMEM] * 12,
        *heads,
        *outs,
        resid,
        attn_gain[None, :],
        ffn_gain[None, :],
        place,
        name="project",
    )
    arrived = [outgoing[0]] + [permuted(outgoing[k], "sp", k) for k in range(1, experts)]
    size = 2 * capacity
    joined = [
        call(
            join_body, sds((size, width)), [VMEM] * 2, arrived[2 * j], arrived[2 * j + 1],
            name="join",
        )
        for j in hops
    ]
    joined += [permuted(item, "tp", 2) for item in joined]
    blocks = joined + [permuted(item, "tp", 1) for item in joined]
    hidden_width = expert_gate.shape[2]
    held = experts * size
    keep, send = call(
        functools.partial(expert_body, blocks=2 * experts, tile=256, down_tile=512),
        (sds((held, width)), sds((held, width))),
        [ANY] * (2 * experts + 3),
        *blocks,
        expert_gate,
        expert_up,
        expert_down,
        scratch=[
            pltpu.VMEM((2 * held, width), BF16),
            pltpu.VMEM((width, hidden_width), BF16),
            pltpu.VMEM((width, hidden_width), BF16),
            pltpu.VMEM((hidden_width, width), BF16),
            pltpu.VMEM((2 * held, hidden_width), BF16),
            pltpu.SemaphoreType.DMA((2 * experts,)),
            pltpu.SemaphoreType.DMA((hidden_width // 128,)),
            pltpu.SemaphoreType.DMA((hidden_width // 128,)),
            pltpu.SemaphoreType.DMA((1,)),
        ],
        name="experts",
        flops=9 * 10**9,
        data=2 * 10**7,
        limit=60 * 2**20,
    )
    received = permuted(send, "tp", 1)
    summed = call(
        add_body,
        tuple(sds((size, width)) for _ in range(experts)),
        [VMEM] * 2,
        keep,
        received,
        name="add",
    )
    returned = [None] * experts
    for j in reversed(hops):
        across = permuted(summed[experts // 2 + j], "tp", 2)
        pair = call(
            split_body,
            (sds((capacity, width)), sds((capacity, width))),
            [VMEM] * 2,
            summed[j],
            across,
            name="split",
        )
        for i in range(2):
            k = 2 * j + i
            returned[k] = permuted(pair[i], "sp", k) if k else pair[i]
    return call(
        finish_body,
        sds((rows, width)),
        [VMEM] * (experts + 3),
        weigh,
        stream,
        moe_gain[None, :],
        *returned,
        scratch=[pltpu.VMEM((experts * capacity, width), BF16)],
        name="finish",
    )


def solution(mesh):
    in_specs = (
        P(("sp", "tp"), None),
        P("sp", "tp"),
        P("sp", "tp"),
        P("sp", None),
        P("sp", None),
        P(),
        P(),
        P(),
        P(),
        P(),
        P("tp", None),
        P("tp", None),
        P(),
        P(),
        P(),
        P(("sp", "tp"), None),
        P(("sp", "tp"), None),
        P("sp", None, "tp"),
        P("sp", None, "tp"),
        P("sp", "tp", None),
    )
    out_specs = P(("sp", "tp"), None)
    direct = mesh.shape["sp"] <= 8 and mesh.shape["tp"] == 4
    local = local_permuted if direct else local_plain
    return jax.shard_map(local, mesh=mesh, in_specs=in_specs, out_specs=out_specs, check_vma=False)
```

```python
import functools

import jax
import jax.numpy as jnp
import numpy as np
from jax import lax
from jax.experimental import pallas as pl
from jax.experimental.pallas import tpu as pltpu
from jax.sharding import PartitionSpec as P


NOPE_W = 128
V_W = 128
NOPE_N = 64
V_N = 64
ROPE = 64

EPS = 1e-06
THETA = 10000.0
LOG2E = 1.4426950408889634
BF16 = jnp.bfloat16
F32 = jnp.float32


def rms_scale(values, gain):
    return values * lax.rsqrt(jnp.mean(values * values, axis=-1, keepdims=True) + EPS) * gain


def rotate(values, positions):
    half = values.shape[-1] // 2
    freq = THETA ** (-jnp.arange(half, dtype=jnp.float32) * 2.0 / values.shape[-1])
    angle = positions.astype(jnp.float32)[..., None] * freq
    cosine = jnp.cos(angle)
    sine = jnp.sin(angle)
    real = values.astype(jnp.float32)
    first = real[..., :half]
    second = real[..., half:]
    return jnp.concatenate(
        [first * cosine - second * sine, second * cosine + first * sine], axis=-1
    ).astype(jnp.bfloat16)


def contract(left, right):
    return lax.dot_general(
        left, right, (((1,), (1,)), ((), ())), preferred_element_type=jnp.float32
    )


def attend(q_nope, q_rope, k_nope, k_rope, values, factor):
    scores = (contract(q_nope, k_nope) + contract(q_rope, k_rope)) * factor
    top = jnp.max(scores, axis=1, keepdims=True)
    weights = jnp.exp(scores - top)
    weight_sum = jnp.sum(weights, axis=1, keepdims=True)
    summed = jnp.dot(weights.astype(BF16), values, preferred_element_type=F32)
    return (summed / weight_sum).astype(BF16)


def local_plain(
    resid,
    query_wide,
    query_narrow,
    latent,
    rope_key,
    latent_gain,
    key_up_wide,
    value_up_wide,
    key_up_narrow,
    value_up_narrow,
    out_wide,
    out_narrow,
    attn_gain,
    ffn_gain,
    moe_gain,
    routes,
    route_logit,
    expert_gate,
    expert_up,
    expert_down,
):
    tok_rows = latent.shape[0]
    wide_heads = query_wide.shape[1] // (NOPE_W + ROPE)
    narrow_heads = query_narrow.shape[1] // (NOPE_N + ROPE)
    tp_rank = lax.axis_index("tp")
    positions = lax.axis_index("sp") * tok_rows + jnp.arange(tok_rows, dtype=jnp.int32)
    normed = rms_scale(latent.astype(jnp.float32), latent_gain).astype(jnp.bfloat16)
    turned_key = rotate(rope_key, positions)

    def my_columns(weight, count):
        return lax.dynamic_slice_in_dim(weight, tp_rank * count, count, 1)

    latent_rows = lax.all_gather(normed, "sp", axis=0, tiled=True)
    turned_rows = lax.all_gather(turned_key, "sp", axis=0, tiled=True)

    def expand(weight, count):
        return jnp.dot(
            latent_rows, my_columns(weight, count), preferred_element_type=F32
        ).astype(BF16)

    def group(query, heads, nope, value, key_up, value_up):
        query = query.reshape(tok_rows, heads, nope + ROPE)
        turned = rotate(query[:, :, nope:], positions[:, None])
        keys = expand(key_up, heads * nope)
        values = expand(value_up, heads * value)
        return [
            attend(
                query[:, h, :nope],
                turned[:, h],
                keys[:, h * nope : (h + 1) * nope],
                turned_rows,
                values[:, h * value : (h + 1) * value],
                (nope + ROPE) ** (-0.5),
            )
            for h in range(heads)
        ]

    wide_out = jnp.concatenate(
        group(query_wide, wide_heads, NOPE_W, V_W, key_up_wide, value_up_wide), axis=1
    )
    narrow_out = jnp.concatenate(
        group(query_narrow, narrow_heads, NOPE_N, V_N, key_up_narrow, value_up_narrow), axis=1
    )
    row_count = resid.shape[0]
    proj = lax.psum_scatter(
        (
            jnp.dot(wide_out, out_wide, preferred_element_type=jnp.float32)
            + jnp.dot(narrow_out, out_narrow, preferred_element_type=jnp.float32)
        ).astype(jnp.bfloat16),
        "tp",
        scatter_dimension=0,
        tiled=True,
    ).astype(jnp.float32)
    stream = (resid.astype(jnp.float32) + rms_scale(proj, attn_gain)).astype(jnp.bfloat16)
    moe_in = rms_scale(stream.astype(jnp.float32), ffn_gain).astype(jnp.bfloat16)
    top_count = routes.shape[1]
    experts = lax.axis_size("sp")
    capacity = (3 * row_count * top_count + 2 * experts - 1) // (2 * experts)
    chosen = routes.reshape(-1)
    onehot = (chosen[:, None] == jnp.arange(experts, dtype=jnp.int32)[None, :]).astype(jnp.int32)
    before = jnp.cumsum(onehot, axis=0) - onehot
    slot = jnp.sum(before * onehot, axis=1)
    dest = (chosen * capacity + slot).reshape(row_count, top_count)
    slot_ids = jnp.arange(experts * capacity, dtype=jnp.int32)
    placing = jnp.any(slot_ids[:, None, None] == dest[None, :, :], axis=2).astype(jnp.bfloat16)
    outgoing = jnp.dot(placing, moe_in, preferred_element_type=jnp.float32).astype(jnp.bfloat16)
    outgoing = outgoing.reshape(experts, capacity, moe_in.shape[1])
    gathered = lax.all_gather(
        lax.all_to_all(outgoing, "sp", split_axis=0, concat_axis=0, tiled=True),
        "tp",
        axis=0,
        tiled=True,
    )
    flat = gathered.reshape(-1, gathered.shape[2])
    gate = jnp.dot(flat, expert_gate[0], preferred_element_type=jnp.float32)
    upper = jnp.dot(flat, expert_up[0], preferred_element_type=jnp.float32)
    hidden = (jax.nn.silu(gate) * upper).astype(jnp.bfloat16)
    partial_out = jnp.dot(hidden, expert_down[0], preferred_element_type=jnp.float32).reshape(
        gathered.shape
    )
    summed = lax.psum_scatter(
        partial_out.astype(jnp.bfloat16), "tp", scatter_dimension=0, tiled=True
    )
    returned = lax.all_to_all(summed, "sp", split_axis=0, concat_axis=0, tiled=True)
    flat_back = returned.reshape(experts * capacity, returned.shape[2])
    picked = flat_back[dest]
    share = jax.nn.softmax(route_logit, axis=-1)
    branch = jnp.sum(share[:, :, None] * picked.astype(jnp.float32), axis=1)
    return (stream.astype(jnp.float32) + rms_scale(branch, moe_gain)).astype(jnp.bfloat16)


def dot(left, right):
    return jnp.dot(left, right, preferred_element_type=F32)


def sds(shape, dtype=BF16):
    return jax.ShapeDtypeStruct(shape, dtype)


VMEM = pl.BlockSpec(memory_space=pltpu.VMEM)
HBM = pl.BlockSpec(memory_space=pltpu.HBM)


def call(body, outs, ins, *args, scratch=(), flops=10**8, data=10**6, limit=8 * 2**20):
    return pl.pallas_call(
        body,
        out_shape=outs,
        in_specs=ins,
        out_specs=jax.tree.map(lambda _: VMEM, outs),
        scratch_shapes=list(scratch),
        cost_estimate=pl.CostEstimate(flops=flops, bytes_accessed=data, transcendentals=0),
        compiler_params=pltpu.CompilerParams(vmem_limit_bytes=limit),
    )(*args)


def angles(freq, start, count):
    spots = start + lax.broadcasted_iota(jnp.int32, (freq.shape[0], count), 1)
    return spots.astype(F32) * freq


def turn_rows(block, cosine, sine):
    half = block.shape[0] // 2
    first, second = block[:half], block[half:]
    return first * cosine - second * sine, second * cosine + first * sine


def pack_body(*refs):
    *sources, out = refs[:5]
    fetched(sources, refs[5:9], refs[9])
    latent, rope, gain, freq = refs[5:9]
    half = latent.shape[0] // 2
    base = pl.multiple_of((lax.axis_index("tp") % 2) * half, half)
    rows = latent[pl.ds(base, half), :].astype(F32)
    out[:half] = rms_scale(rows, gain[...]).astype(BF16)
    angle = angles(freq[...], lax.axis_index("sp") * latent.shape[0] + base, half)
    keys = rope[:, pl.ds(base, half)].astype(F32)
    first, second = turn_rows(keys, jnp.cos(angle), jnp.sin(angle))
    out[half:, :half] = first.astype(BF16)
    out[half:, half:] = second.astype(BF16)


def stacked(rank, count):
    return np.cumsum((count // 2 + ROPE // 2, NOPE_W + NOPE_N, rank, count)).tolist()


def prepare_body(*refs):
    sources, (stack, place, weigh), copies, sem = refs[:10], refs[10:13], refs[13:23], refs[23]
    fetched(sources, copies, sem)
    *copies, pack = copies
    stack[: pack.shape[0], :] = pack[...]
    key_wide, value_wide, key_narrow, value_narrow, wide, narrow, freq, chosen, logit = copies
    rank, count = key_wide.shape[0], wide.shape[1]
    key_at, value_at, wide_at, narrow_at = stacked(rank, count)
    group = lax.axis_index("tp")
    span = pl.ds(pl.multiple_of(group * NOPE_W, NOPE_W), NOPE_W)
    pair = pl.ds(pl.multiple_of((group // 2) * (2 * NOPE_N), 2 * NOPE_N), 2 * NOPE_N)
    odd = group % 2 == 1

    def narrow_part(ref):
        both = ref[:, pair].astype(F32)
        return jnp.where(odd, both[:, NOPE_N:], both[:, :NOPE_N])

    stack[key_at : key_at + NOPE_W, :rank] = key_wide[:, span].astype(F32).T.astype(BF16)
    stack[key_at + NOPE_W : value_at, :rank] = narrow_part(key_narrow).T.astype(BF16)
    stack[value_at:wide_at, :V_W] = value_wide[:, span]
    stack[value_at:wide_at, V_W : V_W + V_N] = narrow_part(value_narrow).astype(BF16)
    angle = angles(freq[:, :1], lax.axis_index("sp") * count, count)
    cosine, sine = jnp.cos(angle), jnp.sin(angle)
    wide_rows, narrow_rows = wide[...].astype(F32), narrow[...].astype(F32).T
    for query, nope, at in ((wide_rows, NOPE_W, wide_at), (narrow_rows, NOPE_N, narrow_at)):
        first, second = turn_rows(query[nope:], cosine, sine)
        full = jnp.concatenate([query[:nope], first, second], axis=0).T.astype(BF16)
        stack[at : at + count, : nope + ROPE] = full
    experts, capacity, tokens = place.shape
    earlier = (
        lax.broadcasted_iota(jnp.int32, (tokens, tokens), 0)
        < lax.broadcasted_iota(jnp.int32, (tokens, tokens), 1)
    ).astype(F32)
    expert_ids = lax.broadcasted_iota(jnp.int32, (experts, tokens), 0)
    row_ids = lax.broadcasted_iota(jnp.int32, (experts * capacity, tokens), 0)
    named = [(expert_ids == chosen[k : k + 1, :]).astype(F32) for k in range(2)]
    before = dot(named[0] + named[1], earlier)
    logits = [logit[k : k + 1, :] for k in range(2)]
    top = jnp.maximum(logits[0], logits[1])
    raised = [jnp.exp(item - top) for item in logits]
    total = raised[0] + raised[1]
    placed = jnp.zeros(row_ids.shape, F32)
    weighed = jnp.zeros(row_ids.shape, F32)
    for k in range(2):
        slot = jnp.sum(before * named[k], axis=0, keepdims=True).astype(jnp.int32)
        away = chosen[k : k + 1, :] ^ lax.axis_index("sp")
        hit = row_ids == away * capacity + slot
        placed = jnp.where(hit, 1.0, placed)
        weighed = jnp.where(hit, raised[k] / total, weighed)
    place[...] = placed.reshape(place.shape).astype(BF16)
    weigh[...] = weighed.T


def attention_body(*refs, packs):
    blocks = refs[: packs - 1]
    stack, *outs = refs[packs - 1 : packs + 4]
    normed, keys_w, keys_n, values, held = refs[packs + 4 :]
    quarter = ROPE // 2
    half = blocks[0].shape[0] - quarter
    for j, ref in enumerate((stack, *blocks)):
        span = pl.ds(j * half, half)
        normed[span, :] = ref[:half, :]
        turned = ref[half : half + quarter, :]
        for keys, nope in ((keys_w, NOPE_W), (keys_n, NOPE_N)):
            keys[nope : nope + quarter, span] = turned[:, :half]
            keys[nope + quarter : nope + ROPE, span] = turned[:, half:]
    rank, count = normed.shape[1], held.shape[0]
    key_at, value_at, wide_at, narrow_at = stacked(rank, count)
    up = contract(stack[key_at:value_at, :rank], normed[...]).astype(BF16)
    keys_w[:NOPE_W, :] = up[:NOPE_W]
    keys_n[:NOPE_N, :] = up[NOPE_W:]
    values[...] = dot(normed[...], stack[value_at:wide_at, : V_W + V_N]).astype(BF16)
    spans = ((wide_at, keys_w, NOPE_W, 0, V_W), (narrow_at, keys_n, NOPE_N, V_W, V_W + V_N))
    for at, keys, nope, low, high in spans:
        score = dot(stack[at : at + count, : nope + ROPE], keys[...])
        top = jnp.max(score, axis=1, keepdims=True)
        weight = jnp.exp2((score - top) * ((nope + ROPE) ** (-0.5) * LOG2E))
        total = jnp.sum(weight, axis=1, keepdims=True)
        summed = dot(weight.astype(BF16), values[:, low:high])
        held[:, low:high] = (summed / total).astype(BF16)
    rows = outs[0].shape[0]
    for k, out in enumerate(outs):
        at = pl.multiple_of((lax.axis_index("tp") ^ k) * rows, rows)
        out[...] = held[pl.ds(at, rows), :]


def project_body(*refs):
    heads, weights = refs[:4], refs[4:12]
    resid, attn_gain, ffn_gain, place, stream, *outs = refs[12:]
    proj = 0.0
    for k, head in enumerate(heads):
        proj = proj + dot(head[:, :V_W], weights[2 * k][...])
        proj = proj + dot(head[:, V_W:], weights[2 * k + 1][...])
    mixed = (resid[...].astype(F32) + rms_scale(proj, attn_gain[...])).astype(BF16)
    stream[...] = mixed
    moved = rms_scale(mixed.astype(F32), ffn_gain[...]).astype(BF16)
    for k, out in enumerate(outs):
        out[...] = dot(place[k], moved).astype(BF16)


def relay_body(source, out):
    out[...] = source[...]


def hold_body(*refs):
    refs[-1][...] = jnp.zeros(refs[-1].shape, F32)


def hold(*values):
    spec = [VMEM] * len(values)
    return call(hold_body, sds((8, 128), F32), spec, *values)


def join_body(*refs):
    *parts, out = refs
    rows = parts[0].shape[0]
    for k, part in enumerate(parts):
        out[k * rows : (k + 1) * rows, :] = part[...]


def expert_body(*refs, tile, down_tile):
    parts = refs[:2]
    shares = (refs[2:5], refs[5:8])
    _, mine, other, rows, hidden = refs[8:]
    size = parts[0].shape[0]
    width = hidden.shape[1] // 2
    for j, ref in enumerate(parts):
        rows[pl.ds(j * size, size), :] = ref[...]
    for k, (gate, up, _) in enumerate(shares):
        for at in range(0, width, tile):
            count = min(tile, width - at)
            left = dot(rows[...], gate[0, :, pl.ds(at, count)])
            right = dot(rows[...], up[0, :, pl.ds(at, count)])
            hidden[:, pl.ds(k * width + at, count)] = (left * jax.nn.sigmoid(left) * right).astype(BF16)
    for at in range(0, rows.shape[1], down_tile):
        span = pl.ds(at, down_tile)
        total = dot(hidden[:, :width], shares[0][2][0, :, span])
        total = (total + dot(hidden[:, width:], shares[1][2][0, :, span])).astype(BF16)
        mine[:, span] = total[:size]
        other[:, span] = total[size:]


def split_body(mine, other, first, second):
    total = (mine[...].astype(F32) + other[...].astype(F32)).astype(BF16)
    rows = first.shape[0]
    first[...] = total[:rows]
    second[...] = total[rows:]


def finish_body(weigh, stream, gain, *refs):
    *blocks, out, full = refs
    rows = blocks[0].shape[0]
    for k, ref in enumerate(blocks):
        full[k * rows : (k + 1) * rows, :] = ref[...]
    whole = weigh[...]
    high = whole.astype(BF16)
    low = (whole - high.astype(F32)).astype(BF16)
    branch = dot(high, full[...]) + dot(low, full[...])
    out[...] = (stream[...].astype(F32) + rms_scale(branch, gain[...])).astype(BF16)


def permuted(value, axis, step):
    size = lax.axis_size(axis)
    return lax.ppermute(value, axis, [(i, i ^ step) for i in range(size)])


def fetched(refs, copies, sem):
    moves = [
        pltpu.make_async_copy(ref, copy, sem.at[i])
        for i, (ref, copy) in enumerate(zip(refs, copies, strict=True))
    ]
    for move in moves:
        move.start()
    for move in moves:
        move.wait()


def like(value):
    return pltpu.VMEM(value.shape, value.dtype)


def local_permuted(
    resid,
    query_wide,
    query_narrow,
    latent,
    rope_key,
    latent_gain,
    key_up_wide,
    value_up_wide,
    key_up_narrow,
    value_up_narrow,
    out_wide,
    out_narrow,
    attn_gain,
    ffn_gain,
    moe_gain,
    routes,
    route_logit,
    expert_gate,
    expert_up,
    expert_down,
):
    experts = lax.axis_size("sp")
    tokens = latent.shape[0]
    width = resid.shape[1]
    rows = resid.shape[0]
    top_count = routes.shape[1]
    capacity = (3 * rows * top_count + 2 * experts - 1) // (2 * experts)
    half = tokens // 2
    hops = range(experts // 2)
    freq = jnp.asarray(
        np.repeat((THETA ** (-np.arange(ROPE // 2) * 2.0 / ROPE))[:, None], half, 1), F32
    )

    sources = (latent, rope_key.T, latent_gain[None, :], freq)
    pack = call(
        pack_body,
        sds((half + ROPE // 2, latent.shape[1])),
        [HBM] * len(sources),
        *sources,
        scratch=[like(item) for item in sources] + [pltpu.SemaphoreType.DMA((len(sources),))],
        limit=None,
    )
    columns = [pack] + [permuted(pack, "sp", 2 * j) for j in hops[1:]]

    shares = (expert_gate, expert_up, expert_down)
    shares += tuple(permuted(item, "tp", 1) for item in shares)

    across_out = [permuted(out_wide, "tp", 2), permuted(out_narrow, "tp", 2)]
    sources = (
        key_up_wide,
        value_up_wide,
        key_up_narrow,
        value_up_narrow,
        query_wide.T,
        query_narrow,
        freq,
        routes.T,
        route_logit.T,
        pack,
    )
    rank = latent.shape[1]
    stack, place, weigh = call(
        prepare_body,
        (
            sds((pack.shape[0] + NOPE_W + NOPE_N + rank + 2 * tokens, rank)),
            sds((experts, capacity, rows)),
            sds((rows, experts * capacity), F32),
        ),
        [HBM] * len(sources),
        *sources,
        scratch=[like(item) for item in sources] + [pltpu.SemaphoreType.DMA((len(sources),))],
        limit=None,
    )
    columns += [permuted(item, "sp", 1) for item in columns]
    packs = columns + [permuted(item, "tp", 1) for item in columns]
    everyone = experts * tokens
    heads = call(
        functools.partial(attention_body, packs=2 * experts),
        tuple(sds((rows, V_W + V_N)) for _ in range(4)),
        [VMEM] * (2 * experts),
        *packs[1:],
        call(relay_body, sds(stack.shape), [VMEM], stack),
        scratch=[
            pltpu.VMEM((everyone, latent.shape[1]), BF16),
            pltpu.VMEM((NOPE_W + ROPE, everyone), BF16),
            pltpu.VMEM((NOPE_N + ROPE, everyone), BF16),
            pltpu.VMEM((everyone, V_W + V_N), BF16),
            pltpu.VMEM((tokens, V_W + V_N), BF16),
        ],
        flops=10**9,
        limit=16 * 2**20,
    )
    *across_out, mine = lax.optimization_barrier((*across_out, heads[0]))
    outs = [
        out_wide,
        out_narrow,
        permuted(out_wide, "tp", 1),
        permuted(out_narrow, "tp", 1),
        *across_out,
        permuted(across_out[0], "tp", 1),
        permuted(across_out[1], "tp", 1),
    ]
    heads = [mine] + [permuted(heads[k], "tp", k) for k in range(1, 4)]
    stream, *outgoing = call(
        project_body,
        (sds((rows, width)),) + tuple(sds((capacity, width)) for _ in range(experts)),
        [VMEM] * 16,
        *heads,
        *outs,
        resid,
        attn_gain[None, :],
        ffn_gain[None, :],
        place,
    )
    arrived = [outgoing[0]] + [permuted(outgoing[k], "sp", k) for k in range(1, experts)]
    size = 2 * capacity
    hidden_width = expert_gate.shape[2]
    returned = [None] * experts
    held = hold(expert_down)
    for j in hops:
        here = call(join_body, sds((size, width)), [VMEM] * 2, *arrived[2 * j : 2 * j + 2])
        mine, other = call(
            functools.partial(expert_body, tile=256, down_tile=512),
            (sds((size, width)), sds((size, width))),
            [VMEM] * 9,
            here,
            permuted(here, "tp", 2),
            *shares,
            held,
            scratch=[
                pltpu.VMEM((2 * size, width), BF16),
                pltpu.VMEM((2 * size, 2 * hidden_width), BF16),
            ],
            flops=2 * 10**9,
            data=2 * 10**7,
            limit=12 * 2**20,
        )
        pair = call(
            split_body,
            (sds((capacity, width)), sds((capacity, width))),
            [VMEM] * 2,
            mine,
            permuted(other, "tp", 2),
        )
        for k in (2 * j, 2 * j + 1):
            returned[k] = permuted(pair[k % 2], "sp", k) if k else pair[0]
    return call(
        finish_body,
        sds((rows, width)),
        [VMEM] * (experts + 3),
        weigh,
        stream,
        moe_gain[None, :],
        *returned,
        scratch=[pltpu.VMEM((experts * capacity, width), BF16)],
    )


def solution(mesh):
    in_specs = (
        P(("sp", "tp"), None),
        P("sp", "tp"),
        P("sp", "tp"),
        P("sp", None),
        P("sp", None),
        P(),
        P(),
        P(),
        P(),
        P(),
        P("tp", None),
        P("tp", None),
        P(),
        P(),
        P(),
        P(("sp", "tp"), None),
        P(("sp", "tp"), None),
        P("sp", None, "tp"),
        P("sp", None, "tp"),
        P("sp", "tp", None),
    )
    out_specs = P(("sp", "tp"), None)
    direct = mesh.shape["sp"] <= 8 and mesh.shape["tp"] == 4
    local = local_permuted if direct else local_plain
    return jax.shard_map(local, mesh=mesh, in_specs=in_specs, out_specs=out_specs, check_vma=False)
```
